32 devices in a mesh: fs: 8 (over z, x), tp: 4 (over y, core).
Axes of the slice: x: 2, y: 2, z: 4, core: 2. Of those that a mesh axis runs over, the one named last changes fastest.
Arguments:
- tokens: bfloat16 [8192, 2048], P('fs', 'tp'), may hold values from -6 to 6
- recurrence_norm_gain: float32 [2048], replicated, may hold values from 0.1 to 1.9
- output_gate_weight: bfloat16 [2048, 2816], P('fs', 'tp'), may hold values from -0.125 to 0.125
- recurrence_input_weight: bfloat16 [2048, 2816], P('fs', 'tp'), may hold values from -0.125 to 0.125
- convolution_taps: float32 [4, 2816], P(None, 'tp'), may hold values from -3 to 3
- recurrence_gate_weight: bfloat16 [8, 352, 352], P('tp'), may hold values from -0.3125 to 0.3125
- input_gate_weight: bfloat16 [8, 352, 352], P('tp'), may hold values from -0.3125 to 0.3125
- base_decay_logit: float32 [2816], P('tp'), may hold values from 4.5 to 9.5
- token_log_decay: float32 [8192], P('fs'), may hold values from -0.7 to 0, as said below
- recurrence_output_weight: bfloat16 [2816, 2048], P('tp', 'fs'), may hold values from -0.4375 to 0.4375
- feedforward_norm_gain: float32 [2048], replicated, may hold values from 0.1 to 1.9
- feedforward_gate_weight: bfloat16 [2048, 5632], P('fs', 'tp'), may hold values from -0.125 to 0.125
- feedforward_up_weight: bfloat16 [2048, 5632], P('fs', 'tp'), may hold values from -0.125 to 0.125
- feedforward_down_weight: bfloat16 [5632, 2048], P('tp', 'fs'), may hold values from -0.15625 to 0.15625
Outputs:
- layer_out: bfloat16 [8192, 2048], P('fs', 'tp')
The draws below stay inside these ranges and needn't reach their ends.
Inputs may be any that keep to these rules, and one draw needn't show every extreme that they name: `token_log_decay`: each entry is zero or lies between -0.7 and -0.22.
All inputs are finite; a program needn't handle non-finite values.
Results may differ from the reference program's by a relative error of at most 0.022.
Values may be sent and summed in bfloat16 or wider, within the bound.
A program may use at most 128 MiB of HBM per device.

```python
import jax
import jax.numpy as jnp
from jax import lax

D = 2048
R = 2816
BW = 352
FF = 5632
CONV = 4
LEN = 128
BLOCKS = 8
TOKENS = 8192
N_TP = 4


def draw_base_decay_logit(key, part):
    keys = jax.random.split(jax.random.fold_in(key, 11), 3)
    slower = jax.random.bernoulli(keys[0], 0.5, (R,))
    fast_values = jax.random.uniform(keys[1], (R,), jnp.float32, 4.5, 5.5)
    slow_values = jax.random.uniform(keys[2], (R,), jnp.float32, 6.5, 9.0)
    return jnp.where(slower, slow_values, fast_values)


def draw_token_log_decay(key, part):
    keys = jax.random.split(jax.random.fold_in(key, 23), 2)
    struck = jax.random.bernoulli(keys[0], 3.0 / LEN, (TOKENS,))
    depths = jax.random.uniform(keys[1], (TOKENS,), jnp.float32, -0.7, -0.22)
    return jnp.where(struck, depths, jnp.zeros((TOKENS,), jnp.float32))


def levels(stream_key, extent, shards, smallest, largest):
    loudness, own = 1.0, jax.random.fold_in(stream_key, 6)
    for axis_at, shards_of in shards:
        heights = jnp.exp(jax.random.uniform(jax.random.fold_in(own, axis_at), (shards_of,), jnp.float32, smallest / len(shards), largest / len(shards)))
        loudness = loudness * jnp.repeat(heights, extent[axis_at] // shards_of).reshape([-1 if axis == axis_at else 1 for axis in range(len(extent))])
    return loudness


def scatter_about(key, dims, deviation, limit, pieces=(), kind=jnp.bfloat16):
    entries = jax.random.normal(key, dims, jnp.float32) * deviation
    if len(pieces) > 0:
        entries = levels(key, dims, pieces, -0.22, 0.18) * entries
    return jnp.clip(entries, min=-limit, max=limit).astype(kind)


def setup_inputs(seed: int = 0) -> dict:
    arg_keys = jax.random.split(jax.random.key(seed), 15)
    return {
        "tokens": scatter_about(arg_keys[0], (TOKENS, D), 1.0, 6.0, ((0, 8), (1, 4))),
        "recurrence_norm_gain": jnp.clip(1.0 + 0.18 * jax.random.normal(arg_keys[1], (D,), jnp.float32), 0.1, 1.9),
        "output_gate_weight": scatter_about(arg_keys[2], (D, R), D ** -0.5, 0.125, ((0, 8), (1, 4))),
        "recurrence_input_weight": scatter_about(arg_keys[3], (D, R), D ** -0.5, 0.125, ((0, 8), (1, 4))),
        "convolution_taps": scatter_about(arg_keys[4], (CONV, R), CONV ** -0.5, 3.0, ((1, 4),), jnp.float32),
        "recurrence_gate_weight": scatter_about(arg_keys[5], (BLOCKS, BW, BW), BW ** -0.5, 0.3125, ((0, 4),)),
        "input_gate_weight": scatter_about(arg_keys[6], (BLOCKS, BW, BW), BW ** -0.5, 0.3125, ((0, 4),)),
        "base_decay_logit": draw_base_decay_logit(jax.random.fold_in(arg_keys[14], 71), 0),
        "token_log_decay": draw_token_log_decay(jax.random.fold_in(arg_keys[14], 71), 0),
        "recurrence_output_weight": scatter_about(arg_keys[9], (R, D), (R // 16) ** -0.5, 0.4375, ((0, 4), (1, 8))),
        "feedforward_norm_gain": jnp.clip(1.0 + 0.18 * jax.random.normal(arg_keys[10], (D,), jnp.float32), 0.1, 1.9),
        "feedforward_gate_weight": scatter_about(arg_keys[11], (D, FF), D ** -0.5, 0.125, ((0, 8), (1, 4))),
        "feedforward_up_weight": scatter_about(arg_keys[12], (D, FF), D ** -0.5, 0.125, ((0, 8), (1, 4))),
        "feedforward_down_weight": scatter_about(arg_keys[13], (FF, D), (FF // 4) ** -0.5, 0.15625, ((0, 4), (1, 8))),
    }


EPSILON = 1e-06
GATE_EXPONENT = 8.0

def norm_rows(values, gain_vec):
    widened = values.astype(jnp.float32)
    scaled = widened * lax.rsqrt(lax.optimization_barrier(jnp.mean(widened * widened, axis=-1, keepdims=True)) + EPSILON)
    return (scaled * gain_vec).astype(jnp.bfloat16)

def causal_taps(feature_vector, convolution_taps, length):
    row_count, channels = feature_vector.shape
    blocks = feature_vector.astype(jnp.float32).reshape(row_count // length, length, channels)
    tap_count = convolution_taps.shape[0]
    padded = jnp.pad(blocks, ((0, 0), (tap_count - 1, 0), (0, 0)))
    summed = jnp.zeros_like(blocks)
    for offset in range(tap_count):
        summed = summed + convolution_taps[offset] * padded[:, offset:offset + length]
    return summed.reshape(row_count, channels).astype(jnp.bfloat16)

def combine_steps(earlier, latter):
    return (earlier[0] * latter[0], latter[0] * earlier[1] + latter[1])

def linear_scan(decays, driven, length):
    row_count, channels = decays.shape
    shaped = (decays.reshape(row_count // length, length, channels), driven.reshape(row_count // length, length, channels))
    result = lax.associative_scan(combine_steps, shaped, axis=1)
    return result[1].reshape(row_count, channels)

def block_map(mixed_in, weight):
    row_count = mixed_in.shape[0]
    shaped = mixed_in.astype(jnp.float32).reshape(row_count, BLOCKS, BW)
    return jnp.einsum('tnd,nde->tne', shaped, weight.astype(jnp.float32)).reshape(row_count, R)

def grouped_product(values, weight, group_count):
    step_size = values.shape[1] // group_count
    summed = jnp.zeros((values.shape[0], weight.shape[1]), jnp.float32)
    for group_index in range(group_count):
        lower = group_index * step_size
        partial_product = jnp.dot(values[:, lower:lower + step_size], weight[lower:lower + step_size], preferred_element_type=jnp.float32).astype(jnp.bfloat16)
        summed = summed + lax.optimization_barrier(partial_product).astype(jnp.float32)
    return summed

def reference(tokens, recurrence_norm_gain, output_gate_weight, recurrence_input_weight, convolution_taps, recurrence_gate_weight, input_gate_weight, base_decay_logit, token_log_decay, recurrence_output_weight, feedforward_norm_gain, feedforward_gate_weight, feedforward_up_weight, feedforward_down_weight):
    normed = norm_rows(tokens, recurrence_norm_gain)
    gate_projected = jnp.dot(normed, output_gate_weight, preferred_element_type=jnp.float32)
    feature_vector = jnp.dot(normed, recurrence_input_weight, preferred_element_type=jnp.float32).astype(jnp.bfloat16)
    mixed_in = causal_taps(feature_vector, convolution_taps, LEN)
    recurrence_gate = jax.nn.sigmoid(block_map(mixed_in, recurrence_gate_weight))
    inject_gate = jax.nn.sigmoid(block_map(mixed_in, input_gate_weight))
    decay_log_value = -GATE_EXPONENT * jax.nn.softplus(-base_decay_logit)[None, :] * recurrence_gate + token_log_decay[:, None]
    decays = jnp.exp(decay_log_value)
    driven = jnp.sqrt(-jnp.expm1(2.0 * decay_log_value)) * (inject_gate * mixed_in.astype(jnp.float32))
    states = linear_scan(decays, driven, LEN)
    carried = (states * jax.nn.gelu(gate_projected)).astype(jnp.bfloat16)
    mixer_sum = grouped_product(carried, recurrence_output_weight, N_TP)
    residual = (tokens.astype(jnp.float32) + mixer_sum).astype(jnp.bfloat16)
    normed_two = norm_rows(residual, feedforward_norm_gain)
    gate_hidden = jnp.dot(normed_two, feedforward_gate_weight, preferred_element_type=jnp.float32)
    up_hidden = jnp.dot(normed_two, feedforward_up_weight, preferred_element_type=jnp.float32)
    hidden = (jax.nn.silu(gate_hidden) * up_hidden).astype(jnp.bfloat16)
    hidden_sum = grouped_product(hidden, feedforward_down_weight, N_TP)
    return (residual.astype(jnp.float32) + hidden_sum).astype(jnp.bfloat16)
```

```python
import functools

import jax
import jax.numpy as jnp
from jax import lax
from jax.experimental import pallas as pl
from jax.experimental.pallas import tpu as pltpu
from jax.sharding import PartitionSpec as P


LEN = 128
EPSILON = 1e-06
GATE_EXPONENT = 8.0


def ring_order(count):
    return tuple(range(0, count, 2)) + tuple(range(count - 1, 0, -2))


def ring_tables(count):
    order = ring_order(count)
    place = [0] * count
    for spot, index in enumerate(order):
        place[index] = spot
    shifts = [0]
    for step in range(1, count // 2):
        shifts += [-step, step]
    shifts.append(count // 2)
    table = [[order[(place[index] + shift) % count] for shift in shifts] for index in range(count)]
    return jnp.array(table, jnp.int32)[lax.axis_index("fs")]


def ring_gather(piece, count):
    order = ring_order(count)
    right = [(order[i], order[(i + 1) % count]) for i in range(count)]
    left = [(order[i], order[(i - 1) % count]) for i in range(count)]

    def hop(value, pairs):
        return lax.ppermute(value, "fs", pairs)

    found = [piece]
    forward = backward = piece
    half = count // 2
    for _ in range(1, half):
        forward = hop(forward, right)
        backward = hop(backward, left)
        found += [forward, backward]
    cut = piece.shape[0] // 2
    found.append(hop(forward[:cut], right))
    found.append(hop(backward[cut:], left))
    return found


def collect(owners_ref, pieces, whole_ref):
    rows = pieces[0].shape[1]
    for k, piece in enumerate(pieces[:-2]):
        spot = pl.ds(pl.multiple_of(owners_ref[k] * rows, rows), rows)
        for lead in range(2):
            whole_ref[lead, spot, :] = piece[lead]
    spot = pl.ds(pl.multiple_of(owners_ref[len(pieces) - 2] * rows, rows), rows)
    for lead in range(2):
        whole_ref[lead, spot, :] = pieces[len(pieces) - 2 + lead][0]


def norm_block(values_ref, gain_ref):
    widened = values_ref[...].astype(jnp.float32)
    scaled = widened * lax.rsqrt(jnp.mean(widened * widened, axis=-1, keepdims=True) + EPSILON)
    return (scaled * gain_ref[...]).astype(jnp.bfloat16)


ROWS = 2 * LEN
ORDERED = pltpu.CompilerParams(dimension_semantics=("arbitrary",), vmem_limit_bytes=60 * 1024 * 1024)


def once(shape):
    zeros = (0,) * len(shape)
    return pl.BlockSpec(shape, lambda i, *_: zeros, pipeline_mode=pl.Buffered(1))


def block_dense(weight):
    groups, block_width, _ = weight.shape
    identity = jnp.eye(groups, dtype=jnp.bfloat16)[:, None, :, None]
    return (weight[:, :, None, :] * identity).reshape(groups * block_width, groups * block_width)


def shift_down(values, amount, place, fill):
    return jnp.where(place >= amount, pltpu.roll(values, amount, 0), fill)


def mixer_kernel(owners_ref, rows_ref, gain_ref, taps_ref, recur_ref, inject_ref, rate_ref, token_ref, *rest):
    pieces, (out_ref, whole_ref) = rest[:-2], rest[-2:]

    @pl.when(pl.program_id(0) == 0)
    def _():
        collect(owners_ref, pieces, whole_ref)

    normed = norm_block(rows_ref, gain_ref)
    feature = jnp.dot(normed, whole_ref[1], preferred_element_type=jnp.float32)
    feature = feature.astype(jnp.bfloat16).astype(jnp.float32)
    place = lax.rem(lax.broadcasted_iota(jnp.int32, feature.shape, 0), LEN)
    taps = taps_ref[...]
    tap_count = taps.shape[0]
    summed = None
    for k in range(tap_count):
        amount = tap_count - 1 - k
        moved = shift_down(feature, amount, place, 0.0) if amount else feature
        term = taps[k : k + 1] * moved
        summed = term if summed is None else summed + term
    mixed = summed.astype(jnp.bfloat16)
    recur = jax.nn.sigmoid(jnp.dot(mixed, recur_ref[...], preferred_element_type=jnp.float32))
    inject = jax.nn.sigmoid(jnp.dot(mixed, inject_ref[...], preferred_element_type=jnp.float32))
    log_decay = rate_ref[...] * recur + token_ref[...]
    decay = jnp.exp(log_decay)
    y = 2.0 * log_decay
    series = -y * (
        1.0 + y * (1 / 2) * (1.0 + y * (1 / 3) * (1.0 + y * (1 / 4) * (1.0 + y * (1 / 5) * (1.0 + y * (1 / 6)))))
    )
    loss = jnp.where(y > -0.25, series, 1.0 - decay * decay)
    state = jnp.sqrt(loss) * (inject * mixed.astype(jnp.float32))
    amount = 1
    while amount < LEN:
        state = state + decay * shift_down(state, amount, place, 0.0)
        if 2 * amount < LEN:
            decay = decay * shift_down(decay, amount, place, 1.0)
        amount *= 2
    gate = jnp.dot(normed, whole_ref[0], preferred_element_type=jnp.float32)
    out_ref[...] = (state * jax.nn.gelu(gate)).astype(jnp.bfloat16)


def mixer(owners, full_rows, gain, taps, recur_weight, inject_weight, base_decay_logit, token_log_decay, pieces):
    rows, width = full_rows.shape
    channels = pieces[0].shape[-1]
    rate = -GATE_EXPONENT * jax.nn.softplus(-base_decay_logit)[None, :]
    block = lambda cols: pl.BlockSpec((ROWS, cols), lambda i, *_: (i, 0))
    return pl.pallas_call(
        mixer_kernel,
        grid_spec=pltpu.PrefetchScalarGridSpec(
            num_scalar_prefetch=1,
            grid=(rows // ROWS,),
            in_specs=[
                block(width),
                once((1, width)),
                once(taps.shape),
                once((channels, channels)),
                once((channels, channels)),
                once((1, channels)),
                block(1),
            ]
            + [once(piece.shape) for piece in pieces],
            out_specs=block(channels),
            scratch_shapes=[pltpu.VMEM((2, width, channels), jnp.bfloat16)],
        ),
        out_shape=jax.ShapeDtypeStruct((rows, channels), jnp.bfloat16),
        compiler_params=ORDERED,
        cost_estimate=pl.CostEstimate(
            flops=4 * rows * channels * (channels + width), bytes_accessed=4 * width * channels, transcendentals=0
        ),
    )(
        owners,
        full_rows,
        gain[None],
        taps,
        block_dense(recur_weight),
        block_dense(inject_weight),
        rate,
        token_log_decay[:, None],
        *pieces,
    )


def hidden_kernel(owners_ref, rows_ref, gain_ref, *rest):
    pieces, (out_ref, whole_ref) = rest[:-2], rest[-2:]

    @pl.when(pl.program_id(0) == 0)
    def _():
        collect(owners_ref, pieces, whole_ref)

    normed = norm_block(rows_ref, gain_ref)
    gate = jnp.dot(normed, whole_ref[0], preferred_element_type=jnp.float32)
    up = jnp.dot(normed, whole_ref[1], preferred_element_type=jnp.float32)
    out_ref[...] = (jax.nn.silu(gate) * up).astype(jnp.bfloat16)


def hidden_units(owners, full_rows, gain, pieces):
    rows, width = full_rows.shape
    units = pieces[0].shape[-1]
    block = lambda cols: pl.BlockSpec((ROWS, cols), lambda i, *_: (i, 0))
    return pl.pallas_call(
        hidden_kernel,
        grid_spec=pltpu.PrefetchScalarGridSpec(
            num_scalar_prefetch=1,
            grid=(rows // ROWS,),
            in_specs=[block(width), once((1, width))] + [once(piece.shape) for piece in pieces],
            out_specs=block(units),
            scratch_shapes=[pltpu.VMEM((2, width, units), jnp.bfloat16)],
        ),
        out_shape=jax.ShapeDtypeStruct((rows, units), jnp.bfloat16),
        compiler_params=ORDERED,
        cost_estimate=pl.CostEstimate(
            flops=4 * rows * units * width, bytes_accessed=4 * width * units, transcendentals=0
        ),
    )(owners, full_rows, gain[None], *pieces)


def down_kernel(groups, where_ref, values_ref, *rest):
    pieces, (mine_ref, other_ref) = rest[:-2], rest[-2:]
    values = values_ref[...]
    cols = pieces[0].shape[1]
    width = mine_ref.shape[2]
    y, core = where_ref[len(pieces)], where_ref[len(pieces) + 1]
    for k, piece in enumerate(pieces):
        term = jnp.dot(values, piece[...], preferred_element_type=jnp.float32).astype(jnp.bfloat16)
        start = where_ref[k] * cols
        target = start // width
        offset = pl.multiple_of(lax.rem(start, width), cols)
        turn = lax.rem(target // 2 - y + groups, groups)
        same = lax.rem(target, 2) == core

        @pl.when(same)
        def _():
            mine_ref[turn, :, pl.ds(offset, cols)] = term

        @pl.when(jnp.logical_not(same))
        def _():
            other_ref[turn, :, pl.ds(offset, cols)] = term


def project_down(owners, values, pieces, tp):
    rows, depth = values.shape
    cols = pieces[0].shape[1]
    width = cols * len(pieces) // tp
    groups = tp // 2
    tall = min(rows, 2 * ROWS)
    index = lax.axis_index("tp")
    where = jnp.concatenate([owners, jnp.stack([index // 2, index % 2]).astype(jnp.int32)])
    out_spec = pl.BlockSpec((groups, tall, width), lambda i, *_: (0, i, 0))
    shape = jax.ShapeDtypeStruct((groups, rows, width), jnp.bfloat16)
    return pl.pallas_call(
        functools.partial(down_kernel, groups),
        grid_spec=pltpu.PrefetchScalarGridSpec(
            num_scalar_prefetch=1,
            grid=(rows // tall,),
            in_specs=[pl.BlockSpec((tall, depth), lambda i, *_: (i, 0))] + [once(piece.shape) for piece in pieces],
            out_specs=[out_spec, out_spec],
        ),
        out_shape=[shape, shape],
        compiler_params=ORDERED,
        cost_estimate=pl.CostEstimate(
            flops=2 * rows * depth * cols * len(pieces), bytes_accessed=2 * depth * cols * len(pieces), transcendentals=0
        ),
    )(where, values, *pieces)


def scatter_sum(mine, other, tp):
    groups = tp // 2
    got = lax.ppermute(other, "tp", [(i, i ^ 1) for i in range(tp)])
    widen = lambda value: value.astype(jnp.float32)
    total = None
    for turn in range(1, groups):
        pair = (widen(mine[turn]) + widen(got[turn])).astype(jnp.bfloat16)
        perm = [(i, (i + 2 * turn) % tp) for i in range(tp)]
        arrived = widen(lax.ppermute(pair, "tp", perm))
        total = arrived if total is None else total + arrived
    own = widen(mine[0]) + widen(got[0])
    return own if total is None else own + total


def join_last(pieces):
    return pieces[:-2] + [jnp.concatenate(pieces[-2:], axis=0)]


def shards(
    count,
    tp,
    tokens,
    recurrence_norm_gain,
    output_gate_weight,
    recurrence_input_weight,
    convolution_taps,
    recurrence_gate_weight,
    input_gate_weight,
    base_decay_logit,
    token_log_decay,
    recurrence_output_weight,
    feedforward_norm_gain,
    feedforward_gate_weight,
    feedforward_up_weight,
    feedforward_down_weight,
):
    owners = ring_tables(count)
    first = ring_gather(jnp.stack([output_gate_weight, recurrence_input_weight]), count)
    out_pieces = join_last(ring_gather(recurrence_output_weight, count))
    second = ring_gather(jnp.stack([feedforward_gate_weight, feedforward_up_weight]), count)
    down_pieces = join_last(ring_gather(feedforward_down_weight, count))

    full_rows = lax.all_gather(tokens, "tp", axis=1, tiled=True)
    carried = mixer(
        owners,
        full_rows,
        recurrence_norm_gain,
        convolution_taps,
        recurrence_gate_weight,
        input_gate_weight,
        base_decay_logit,
        token_log_decay,
        first,
    )
    mine, other = project_down(owners, carried, out_pieces, tp)
    own_sum = scatter_sum(mine, other, tp)
    residual_own = (tokens.astype(jnp.float32) + own_sum).astype(jnp.bfloat16)
    residual_full = lax.all_gather(residual_own, "tp", axis=1, tiled=True)
    hidden = hidden_units(owners, residual_full, feedforward_norm_gain, second)
    chunks = 2 if hidden.shape[0] % (2 * ROWS) == 0 else 1
    size = hidden.shape[0] // chunks
    sums = []
    for chunk in range(chunks):
        mine, other = project_down(owners, hidden[chunk * size : (chunk + 1) * size], down_pieces, tp)
        sums.append(scatter_sum(mine, other, tp))
    own_down = jnp.concatenate(sums, axis=0)
    return (residual_own.astype(jnp.float32) + own_down).astype(jnp.bfloat16)


def solution(mesh):
    in_specs = (
        P("fs", "tp"),
        P(),
        P("fs", "tp"),
        P("fs", "tp"),
        P(None, "tp"),
        P("tp", None, None),
        P("tp", None, None),
        P("tp"),
        P("fs"),
        P("tp", "fs"),
        P(),
        P("fs", "tp"),
        P("fs", "tp"),
        P("tp", "fs"),
    )
    body = functools.partial(shards, mesh.shape["fs"], mesh.shape["tp"])
    return jax.shard_map(body, mesh=mesh, in_specs=in_specs, out_specs=P("fs", "tp"), check_vma=False)
```
